512 devices in a mesh: sp: 64 (over z, y), tp: 8 (over x, core).
Axes of the slice: x: 4, y: 4, z: 16, core: 2. Of those that a mesh axis runs over, the one named last changes fastest.
Arguments:
- tokens: bfloat16 [6144, 4, 1024], P(('sp', 'tp')), may hold values from -6 to 6
- in_gain: float32 [1024], replicated, may hold values from 0.1 to 1.9
- w_query: bfloat16 [1024, 1024], P('sp', 'tp'), may hold values from -0.1875 to 0.1875
- w_key: bfloat16 [1024, 1024], P('sp', 'tp'), may hold values from -0.1875 to 0.1875
- w_value: bfloat16 [1024, 1024], P('sp', 'tp'), may hold values from -0.1875 to 0.1875
- w_gate: bfloat16 [1024, 1024], P('sp', 'tp'), may hold values from -0.1875 to 0.1875
- w_beta: bfloat16 [1024, 8], P('sp', 'tp'), may hold values from -0.1875 to 0.1875
- conv_query: bfloat16 [4, 1024], P(None, 'tp'), may hold values from -3 to 3
- conv_key: bfloat16 [4, 1024], P(None, 'tp'), may hold values from -3 to 3
- conv_value: bfloat16 [4, 1024], P(None, 'tp'), may hold values from -3 to 3
- decay_rate: float32 [8], P('tp'), may hold values from 0.1 to 3
- out_gain: float32 [128], replicated, may hold values from 0.1 to 1.9
- w_out: bfloat16 [1024, 1024], P('tp', 'sp'), may hold values from -0.1875 to 0.1875
Outputs:
- mixed: bfloat16 [6144, 4, 1024], P(('sp', 'tp'))
The draws below stay inside these ranges and needn't reach their ends.
All inputs are finite; a program needn't handle non-finite values.
Results may differ from the reference program's by a relative error of at most 0.02.
Values may be sent and summed in bfloat16 or wider, within the bound.
No kernel may reach another device: no remote copies, remote signals or barrier semaphores. Data moves between devices by JAX's collectives and lax.ppermute only.
A program may use at most 64 MiB of HBM per device.

```python
import math
import jax
import jax.numpy as jnp
from jax import lax

D = 1024
HEADS = 8
DK = 128
CONV_K = 4
BLOCK = 32
SEQS = 4
TOKENS = 6144


def shard_levels(own_key, extent, shards, low, top_value):
    level, own = 1.0, jax.random.fold_in(own_key, 6)
    for dim, parts in shards:
        heights = jnp.exp(jax.random.uniform(jax.random.fold_in(own, dim), (parts,), jnp.float32, low / len(shards), top_value / len(shards)))
        level = level * jnp.repeat(heights, extent[dim] // parts).reshape([-1 if axis == dim else 1 for axis in range(len(extent))])
    return level


def normal_values(stream_key, shape, spread, limit, shards=(), held_as=jnp.bfloat16):
    values = spread * jax.random.normal(stream_key, shape, jnp.float32)
    if shards:
        values = values * shard_levels(stream_key, shape, shards, -0.22, 0.18)
    return jnp.clip(values, -limit, limit).astype(held_as)


def setup_inputs(seed: int = 0) -> dict:
    key_of = jax.random.split(jax.random.key(seed), 14)
    tokens = normal_values(key_of[0], (TOKENS, SEQS, D), 1.0, 6.0, ((0, 512),))
    in_gain = jnp.clip(1.0 + 0.18 * jax.random.normal(key_of[1], (D,), jnp.float32), 0.1, 1.9)
    w_query = normal_values(key_of[2], (D, HEADS * DK), D ** -0.5, 0.1875, ((0, 64), (1, 8)))
    w_key = normal_values(key_of[3], (D, HEADS * DK), D ** -0.5, 0.1875, ((0, 64), (1, 8)))
    w_value = normal_values(key_of[4], (D, HEADS * DK), D ** -0.5, 0.1875, ((0, 64), (1, 8)))
    w_gate = normal_values(key_of[5], (D, HEADS * DK), D ** -0.5, 0.1875, ((0, 64), (1, 8)))
    w_beta = normal_values(key_of[6], (D, HEADS), D ** -0.5, 0.1875, ((0, 64), (1, 8)))
    conv_query = normal_values(key_of[7], (CONV_K, HEADS * DK), CONV_K ** -0.5, 3.0, ((1, 8),))
    conv_key = normal_values(key_of[8], (CONV_K, HEADS * DK), CONV_K ** -0.5, 3.0, ((1, 8),))
    conv_value = normal_values(key_of[9], (CONV_K, HEADS * DK), CONV_K ** -0.5, 3.0, ((1, 8),))
    decay_rate = jnp.clip(jnp.exp(math.log(3.0) - 3.4011974 * jax.random.uniform(key_of[10], (HEADS,), jnp.float32) ** shard_levels(key_of[10], (HEADS,), ((0, 8),), -0.2, 0.2)), 0.1, 3.0)
    out_gain = jnp.clip(1.0 + 0.18 * jax.random.normal(key_of[11], (DK,), jnp.float32), 0.1, 1.9)
    w_out = normal_values(key_of[12], (HEADS * DK, D), (HEADS * DK) ** -0.5, 0.1875, ((0, 8), (1, 64)))
    return {"tokens": tokens, "in_gain": in_gain, "w_query": w_query, "w_key": w_key, "w_value": w_value, "w_gate": w_gate, "w_beta": w_beta, "conv_query": conv_query, "conv_key": conv_key, "conv_value": conv_value, "decay_rate": decay_rate, "out_gain": out_gain, "w_out": w_out}


epsilon = 1e-06
out_epsilon = 1e-10
highest = lax.Precision.HIGHEST

def unit_inverse(lower):
    size = lower.shape[-1]
    inverse = jnp.eye(size, dtype=jnp.float32) - lower
    power = jnp.matmul(lower, lower, precision=highest)
    span = 2
    while span < size:
        inverse = inverse + jnp.matmul(inverse, power, precision=highest)
        power = jnp.matmul(power, power, precision=highest)
        span = span * 2
    return inverse

def make_terms(query, keys, values, beta, rate_col):
    size = query.shape[-2]
    steps = jnp.arange(1, size + 1).astype(jnp.float32)
    cumulative = -rate_col * steps
    lower_mask = jnp.tril(jnp.ones((size, size), bool))
    strict_mask = jnp.tril(jnp.ones((size, size), bool), -1)
    decay = jnp.where(lower_mask, jnp.exp(cumulative[..., :, None] - cumulative[..., None, :]), 0.0)
    weighted = keys * beta[..., None]
    lower = jnp.where(strict_mask, jnp.einsum('...cd,...sd->...cs', weighted, keys, precision=highest) * decay, 0.0)
    inverse = unit_inverse(lower)
    update = jnp.einsum('...cs,...sv->...cv', inverse, values * beta[..., None], precision=highest)
    erase = jnp.einsum('...cs,...sd->...cd', inverse, weighted * jnp.exp(cumulative)[..., None], precision=highest)
    scores = jnp.einsum('...cd,...sd->...cs', query, keys, precision=highest) * decay
    query_decayed = query * jnp.exp(cumulative)[..., None]
    final = cumulative[..., -1:]
    keys_decayed = keys * jnp.exp(final - cumulative)[..., None]
    return (query_decayed, keys_decayed, update, erase, scores, jnp.exp(final))

def apply_block(state, terms):
    query_decayed, keys_decayed, update, erase, scores, kept = terms
    fresh = update - jnp.einsum('...cd,...dv->...cv', erase, state, precision=highest)
    output = jnp.einsum('...cd,...dv->...cv', query_decayed, state, precision=highest)
    output = output + jnp.einsum('...cs,...sv->...cv', scores, fresh, precision=highest)
    state = state * kept[..., None] + jnp.einsum('...cd,...cv->...dv', keys_decayed, fresh, precision=highest)
    return (state, output)

def causal_conv(pre, conv_taps, history):
    width = conv_taps.shape[0]
    extended = jnp.concatenate([history, pre], axis=0).astype(jnp.float32)
    length = pre.shape[0]
    total = jnp.zeros(pre.shape, jnp.float32)
    for tap in range(width):
        total = total + extended[tap:tap + length] * conv_taps[tap].astype(jnp.float32)
    return total

def rms_scale(values_in, gain):
    values = values_in.astype(jnp.float32)
    scaled = values * lax.rsqrt(lax.optimization_barrier(jnp.mean(values * values, axis=-1, keepdims=True)) + epsilon)
    return (scaled * gain).astype(jnp.bfloat16)

def l2_normalize(array):
    return array * lax.rsqrt(lax.optimization_barrier(jnp.sum(array * array, axis=-1, keepdims=True)) + epsilon)

def finish(outputs, out_gain, gate_pre):
    normed = outputs * lax.rsqrt(lax.optimization_barrier(jnp.mean(outputs * outputs, axis=-1, keepdims=True)) + out_epsilon) * out_gain
    gate = jax.nn.silu(gate_pre.astype(jnp.float32)).reshape(outputs.shape)
    return (normed * gate).astype(jnp.bfloat16).reshape(outputs.shape[0], outputs.shape[1], -1)

def reference(tokens, in_gain, w_query, w_key, w_value, w_gate, w_beta, conv_query, conv_key, conv_value, decay_rate, out_gain, w_out):
    width = tokens.shape[2]
    head_width = HEADS * DK
    normed = rms_scale(tokens, in_gain)
    flat = normed.reshape(-1, width)

    def project(weight):
        return jnp.dot(flat, weight, preferred_element_type=jnp.float32).astype(jnp.bfloat16).reshape(TOKENS, SEQS, -1)
    mixed_pre = jnp.concatenate([project(w_query), project(w_key), project(w_value)], axis=2)
    gate_pre = project(w_gate)
    beta_pre = project(w_beta)
    history = jnp.zeros((CONV_K - 1, SEQS, 3 * head_width), jnp.bfloat16)
    conv_taps = jnp.concatenate([conv_query, conv_key, conv_value], axis=1)
    convolved = jax.nn.silu(causal_conv(mixed_pre, conv_taps, history))

    def split_heads(array):
        return array.reshape(TOKENS, SEQS, HEADS, DK)
    query = l2_normalize(split_heads(convolved[:, :, :head_width])) * DK ** (-0.5)
    keys = l2_normalize(split_heads(convolved[:, :, head_width:2 * head_width]))
    values = split_heads(convolved[:, :, 2 * head_width:])
    beta = jax.nn.sigmoid(beta_pre.astype(jnp.float32) + math.log(DK / (4.0 * TOKENS)))
    rate_col = (decay_rate / TOKENS)[:, None]
    blocks = TOKENS // BLOCK

    def to_blocks(array):
        return jnp.moveaxis(array.reshape(blocks, BLOCK, SEQS, HEADS, DK), 1, 3)
    beta_blocks = jnp.moveaxis(beta.reshape(blocks, BLOCK, SEQS, HEADS), 1, 3)

    def advance(state, inputs):
        query_block, key_block, value_block, beta_block = inputs
        return apply_block(state, make_terms(query_block, key_block, value_block, beta_block, rate_col))
    initial = jnp.zeros((SEQS, HEADS, DK, DK), jnp.float32)
    _, outputs = lax.scan(advance, initial, (to_blocks(query), to_blocks(keys), to_blocks(values), beta_blocks))
    outputs = jnp.moveaxis(outputs, 3, 1).reshape(TOKENS, SEQS, HEADS, DK)
    gated = finish(outputs, out_gain, gate_pre)
    mixed = jnp.dot(gated.reshape(-1, head_width), w_out, preferred_element_type=jnp.float32).astype(jnp.bfloat16)
    return mixed.reshape(TOKENS, SEQS, width)
```

```python
import math

import jax
import jax.numpy as jnp
from jax import lax
from jax.experimental import pallas as pl
from jax.experimental.pallas import tpu as pltpu
from jax.sharding import Mesh
from jax.sharding import PartitionSpec as P

Z = ("zh", "zl")
SP = ("zh", "zl", "y")
TP = ("x", "c")
ALL = ("zh", "zl", "y", "x", "c")

EPS = 1e-06
OUT_EPS = 1e-10
LANES = 128
CHUNK = 128
BLOCK = 32
f32 = jnp.float32
bf16 = jnp.bfloat16


def dot(a, b):
    return jnp.dot(a.astype(bf16), b.astype(bf16), preferred_element_type=f32)


def dot_t(a, b):
    return lax.dot_general(
        a.astype(bf16), b.astype(bf16), (((1,), (1,)), ((), ())), preferred_element_type=f32
    )


def dot_l(a, b):
    return lax.dot_general(
        a.astype(bf16), b.astype(bf16), (((0,), (0,)), ((), ())), preferred_element_type=f32
    )


def sigmoid(x):
    return 1.0 / (1.0 + jnp.exp(-x))


def rms_scale(values_in, gain):
    values = values_in.astype(f32)
    scaled = values * lax.rsqrt(jnp.mean(values * values, axis=-1, keepdims=True) + EPS)
    return (scaled * gain).astype(bf16)


def project_kernel(ny, nz, rows, skip, x_ref, w_ref, pre_ref, qkv_ref, out_ref):
    piece = 6 * rows

    def part(k):
        return jnp.concatenate(
            [
                w_ref[y, pl.ds(skip + z * piece + k * rows, rows), :]
                for z in range(nz)
                for y in range(ny)
            ],
            axis=0,
        )

    weights = jnp.concatenate([part(0), part(1), part(2)], axis=1)
    qkv_ref[...] = weights
    x = x_ref[...]
    pre_ref[:, : 3 * LANES] = jnp.dot(x, weights, preferred_element_type=f32).astype(bf16)
    tail = jnp.concatenate([part(3), part(5)], axis=1)
    pre_ref[:, 3 * LANES :] = jnp.dot(x, tail, preferred_element_type=f32).astype(bf16)
    out_ref[...] = part(4)


def delta_kernel(shift, pre_ref, hist_ref, w_ref, taps_ref, par_ref, o_ref, r_ref, eb_ref, ext):
    span = pre_ref.shape[0]
    width = 3 * LANES
    lam = par_ref[0:1, :]
    ext[0:8, :] = (
        jnp.dot(hist_ref[...], w_ref[...], preferred_element_type=f32).astype(bf16).astype(f32)
    )
    ext[8:, :] = pre_ref[:, :width].astype(f32)
    total = ext[5 : 5 + span, :] * taps_ref[0:1, :]
    for tap in range(1, 4):
        total = total + ext[5 + tap : 5 + tap + span, :] * taps_ref[tap : tap + 1, :]
    act = total * sigmoid(total)
    query, keys, values = act[:, :LANES], act[:, LANES : 2 * LANES], act[:, 2 * LANES :]
    query = query * (
        lax.rsqrt(jnp.sum(query * query, axis=-1, keepdims=True) + EPS) * LANES ** (-0.5)
    )
    keys = keys * lax.rsqrt(jnp.sum(keys * keys, axis=-1, keepdims=True) + EPS)
    beta = sigmoid(pre_ref[:, 4 * LANES :].astype(f32) + shift)

    shape = (CHUNK, CHUNK)
    i = lax.broadcasted_iota(jnp.int32, shape, 0)
    j = lax.broadcasted_iota(jnp.int32, shape, 1)
    row = i.astype(f32)
    decay = jnp.where(i >= j, jnp.exp(-lam * (row - j.astype(f32))), 0.0)
    strict = jnp.where(i > j, decay, 0.0)
    gamma = jnp.exp(-lam * (row + 1.0))
    toward = jnp.exp(-lam * (CHUNK - 1.0 - row))
    kept = jnp.exp(-lam * float(CHUNK))
    eye = jnp.where(i == j, 1.0, 0.0)
    same = [(i // s) == (j // s) for s in (BLOCK, 2 * BLOCK)]
    count = span // CHUNK
    ks = [keys[n * CHUNK : (n + 1) * CHUNK] for n in range(count)]
    qs = [query[n * CHUNK : (n + 1) * CHUNK] for n in range(count)]
    vs = [values[n * CHUNK : (n + 1) * CHUNK] for n in range(count)]
    bs = [beta[n * CHUNK : (n + 1) * CHUNK] for n in range(count)]
    kb = [k * b for k, b in zip(ks, bs)]
    lower = [dot_t(a, k) * strict for a, k in zip(kb, ks)]
    diag = [jnp.where(same[0], a, 0.0) for a in lower]
    inv = [eye - a for a in diag]
    power = [dot(a, a) for a in diag]
    reach = 2
    while reach < BLOCK:
        inv = [a + dot(a, p) for a, p in zip(inv, power)]
        reach *= 2
        if reach < BLOCK:
            power = [dot(p, p) for p in power]
    side = [jnp.where(same[1], jnp.where(same[0], 0.0, a), 0.0) for a in lower]
    inv = [a - dot(a, dot(s, a)) for a, s in zip(inv, side)]
    side = [jnp.where(same[1], 0.0, a) for a in lower]
    inv = [a - dot(a, dot(s, a)) for a, s in zip(inv, side)]
    uw = [
        dot(a, jnp.concatenate([v * b, k * gamma], axis=1))
        for a, v, b, k in zip(inv, vs, bs, kb)
    ]
    scores = [dot_t(q, k) * decay for q, k in zip(qs, ks)]
    su = [dot(s, a) for s, a in zip(scores, uw)]
    ku = [dot_l(k * toward, a) for k, a in zip(ks, uw)]
    local = [a[:, :LANES] for a in su]
    read = [q * gamma - a[:, LANES:] for q, a in zip(qs, su)]
    new = [a[:, :LANES] for a in ku]
    drop = [-a[:, LANES:] for a in ku]
    fmap, off = drop[0], new[0]
    o_ref[:CHUNK, :] = local[0]
    r_ref[:CHUNK, :] = read[0].astype(bf16)
    kap = kept
    for n in range(1, count):
        both = jnp.concatenate([fmap, off], axis=1)
        seen = dot(read[n], both)
        at = slice(n * CHUNK, (n + 1) * CHUNK)
        o_ref[at, :] = local[n] + seen[:, LANES:]
        r_ref[at, :] = (read[n] * kap + seen[:, :LANES]).astype(bf16)
        moved = dot(drop[n], both)
        fmap = fmap * kept + drop[n] * kap + moved[:, :LANES]
        off = off * kept + moved[:, LANES:] + new[n]
        kap = kap * kept
    eb_ref[:LANES, :] = fmap.astype(bf16)
    eb_ref[LANES:, :] = off.astype(bf16)


def group_kernel(span, g_ref, par_ref, eb_ref, prefix_ref):
    lam = par_ref[0:1, :]
    place = par_ref[1:2, :]
    count = g_ref.shape[0]
    fmap = jnp.zeros((LANES, LANES), f32)
    off = jnp.zeros((LANES, LANES), f32)
    keep_map, keep_off = fmap, off
    step = jnp.exp(-lam * float(span))
    for m in range(count):
        kap = jnp.exp(-lam * float(span * m))
        e = g_ref[m, :LANES, :]
        if m:
            moved = dot(e, jnp.concatenate([fmap, off], axis=1))
            fmap = fmap * step + e.astype(f32) * kap + moved[:, :LANES]
            off = off * step + moved[:, LANES:] + g_ref[m, LANES:, :].astype(f32)
        else:
            fmap = e.astype(f32)
            off = g_ref[m, LANES:, :].astype(f32)
        if m + 1 < count:
            here = place == float(m + 1)
            keep_map = jnp.where(here, fmap, keep_map)
            keep_off = jnp.where(here, off, keep_off)
    eb_ref[:LANES, :] = fmap.astype(bf16)
    eb_ref[LANES:, :] = off.astype(bf16)
    prefix_ref[:LANES, :] = keep_map
    prefix_ref[LANES:, :] = keep_off


def finish_kernel(span, g_ref, prefix_ref, par_ref, o_ref, r_ref, pre_ref, gain_ref, out_ref):
    lam = par_ref[0:1, :]
    low = par_ref[1:2, :]
    high = par_ref[2:3, :]
    count = g_ref.shape[0]
    step = jnp.exp(-lam * float(span * count))
    state = jnp.where(high > 0.0, g_ref[0, LANES:, :].astype(f32), 0.0)
    for m in range(1, count - 1):
        later = state * step + dot(g_ref[m, :LANES, :], state) + g_ref[m, LANES:, :].astype(f32)
        state = jnp.where(high > float(m), later, state)
    entry = (
        state * jnp.exp(-lam * (low * float(span)))
        + dot(prefix_ref[:LANES, :], state)
        + prefix_ref[LANES:, :]
    )
    out = o_ref[...] + dot(r_ref[...], entry)
    normed = out * lax.rsqrt(jnp.mean(out * out, axis=-1, keepdims=True) + OUT_EPS) * gain_ref[0:1, :]
    gate = pre_ref[:, 3 * LANES : 4 * LANES].astype(f32)
    out_ref[...] = (normed * (gate * sigmoid(gate))).astype(bf16)


def call(kernel, outs, args, flops, scratch=()):
    spec = pl.BlockSpec(memory_space=pltpu.VMEM)
    return pl.pallas_call(
        kernel,
        out_shape=outs,
        in_specs=[spec] * len(args),
        out_specs=tuple([spec] * len(outs)),
        scratch_shapes=scratch,
        cost_estimate=pl.CostEstimate(flops=flops, bytes_accessed=4 << 20, transcendentals=0),
        compiler_params=pltpu.CompilerParams(vmem_limit_bytes=40 << 20),
    )(*args)


def shards(
    tokens,
    in_gain,
    w_query,
    w_key,
    w_value,
    w_gate,
    w_beta,
    conv_query,
    conv_key,
    conv_value,
    decay_rate,
    out_gain,
    w_out,
):
    own, seqs, width = tokens.shape
    rows = w_query.shape[0]
    nz = lax.axis_size("zh") * lax.axis_size("zl")
    ny, nx, nc = lax.axis_size("y"), lax.axis_size("x"), lax.axis_size("c")
    span = own * ny * nx * nc
    total = span * nz
    piece = 6 * rows
    slot = own * width // LANES

    normed = rms_scale(tokens, in_gain)
    pack = jnp.concatenate(
        [
            w_query,
            w_key,
            w_value,
            w_gate,
            w_out.T,
            jnp.broadcast_to(w_beta, (rows, LANES)),
        ],
        axis=0,
    )
    deep = lax.all_gather(pack, Z).reshape(nz * piece, LANES)
    send = jnp.concatenate(
        [
            normed.transpose(1, 0, 2).reshape(seqs, slot, LANES),
            jnp.broadcast_to(deep, (seqs, nz * piece, LANES)),
        ],
        axis=1,
    )
    got = lax.all_to_all(send, "y", 0, 0, tiled=True)
    x = lax.all_gather(got[:, :slot], TP)
    x = x.reshape(nx * nc, ny, own, width).transpose(1, 0, 2, 3).reshape(span, width)
    pairs = [(k, k + 1) for k in range(nz - 1)]
    hist = lax.ppermute(x[span - 8 :], Z, pairs)

    pre, w_qkv, out_rows = call(
        lambda *refs: project_kernel(ny, nz, rows, slot, *refs),
        (
            jax.ShapeDtypeStruct((span, 5 * LANES), bf16),
            jax.ShapeDtypeStruct((width, 3 * LANES), bf16),
            jax.ShapeDtypeStruct((width, LANES), bf16),
        ),
        (x, got),
        2 * span * width * 5 * LANES,
    )
    out_pair = lax.all_gather(out_rows, "c")

    lam = decay_rate.astype(f32) / total
    places = jnp.stack(
        [
            lam[0],
            lax.axis_index("zl").astype(f32),
            lax.axis_index("zh").astype(f32),
        ]
    )
    par = jnp.broadcast_to(jnp.pad(places, (0, 5))[:, None], (8, LANES))
    taps = jnp.concatenate([conv_query, conv_key, conv_value], axis=1).astype(f32)
    taps = jnp.pad(taps, ((0, 4), (0, 0)))
    shift = math.log(LANES / (4.0 * total))
    local, read, eb = call(
        lambda *refs: delta_kernel(shift, *refs),
        (
            jax.ShapeDtypeStruct((span, LANES), f32),
            jax.ShapeDtypeStruct((span, LANES), bf16),
            jax.ShapeDtypeStruct((2 * LANES, LANES), bf16),
        ),
        (pre, hist, w_qkv, taps, par),
        200 << 20,
        (pltpu.VMEM((span + 8, 3 * LANES), f32),),
    )
    group = lax.all_gather(eb, "zl")
    eb_group, prefix = call(
        lambda *refs: group_kernel(span, *refs),
        (
            jax.ShapeDtypeStruct((2 * LANES, LANES), bf16),
            jax.ShapeDtypeStruct((2 * LANES, LANES), f32),
        ),
        (group, par),
        30 << 20,
    )
    groups = lax.all_gather(eb_group, "zh")
    gain = jnp.broadcast_to(out_gain[None, :], (8, LANES))
    (gated,) = call(
        lambda *refs: finish_kernel(span, *refs),
        (jax.ShapeDtypeStruct((span, LANES), bf16),),
        (groups, prefix, par, local, read, pre, gain),
        40 << 20,
    )
    halves = gated.reshape(ny * nx, nc, own, LANES).transpose(1, 0, 2, 3)
    heads = lax.all_to_all(halves, "c", 0, 0, tiled=True).reshape(nc, -1, LANES)
    part = jnp.einsum("ctd,cod->to", heads, out_pair, preferred_element_type=f32).astype(bf16)
    parts = lax.all_to_all(part.reshape(ny * nx, own, width), ("y", "x"), 0, 0, tiled=True)
    mixed = jnp.sum(parts.reshape(ny, nx, own, width).astype(f32), axis=1)
    return mixed.astype(bf16).transpose(1, 0, 2)


def solution(mesh):
    sp, tp = mesh.devices.shape
    finer = Mesh(mesh.devices.reshape(4, sp // 16, 4, tp // 2, 2), ALL)
    return jax.shard_map(
        shards,
        mesh=finer,
        in_specs=(
            P(ALL, None, None),
            P(),
            P(SP, TP),
            P(SP, TP),
            P(SP, TP),
            P(SP, TP),
            P(SP, TP),
            P(None, TP),
            P(None, TP),
            P(None, TP),
            P(TP),
            P(),
            P(TP, SP),
        ),
        out_specs=P(ALL, None, None),
        check_vma=False,
    )
```
